32 devices in a mesh: grp: 2 (over y), tp: 4 (over z), dp: 4 (over x, core).
Axes of the slice: x: 2, y: 2, z: 4, core: 2. Of those that a mesh axis runs over, the one named last changes fastest.
Arguments:
- tokens: bfloat16 [128, 2048], P(('grp', 'tp'), 'dp'), parts along dimension 0, may hold values from -200 to 200
- norm_gain: bfloat16 [2, 2048], P(None, 'dp'), may hold values from 0.099609375 to 1.8984375
- w_z: bfloat16 [2, 2048, 4096], P(None, 'dp', 'tp'), may hold values from -0.125 to 0.125
- w_x: bfloat16 [2, 2048, 4096], P(None, 'dp', 'tp'), may hold values from -0.125 to 0.125
- w_b: bfloat16 [2, 2048, 1024], P(None, 'dp', 'tp'), may hold values from -0.125 to 0.125
- w_c: bfloat16 [2, 2048, 1024], P(None, 'dp', 'tp'), may hold values from -0.125 to 0.125
- w_dt: bfloat16 [2, 2048, 64], P(None, 'dp'), may hold values from -0.125 to 0.125
- conv_x: bfloat16 [2, 4, 4096], P(None, None, 'tp'), may hold values from -3 to 3
- conv_b: bfloat16 [2, 4, 1024], P(None, None, 'tp'), may hold values from -3 to 3
- conv_c: bfloat16 [2, 4, 1024], P(None, None, 'tp'), may hold values from -3 to 3
- dt_bias: float32 [2, 64], P(None, 'tp'), may hold values from -3 to 0.5
- a_log: float32 [2, 64], P(None, 'tp'), may hold values from 0 to 2.5
- d_skip: float32 [2, 64], P(None, 'tp'), may hold values from 0.5 to 2
- out_gain: bfloat16 [2, 4096], P(None, 'tp'), may hold values from 0.099609375 to 1.8984375
- w_out: bfloat16 [2, 4096, 2048], P(None, 'tp', 'dp'), may hold values from -0.09375 to 0.09375
- ssm_state: float32 [2, 128, 64, 64, 64], P(None, ('grp', 'dp'), 'tp'), parts along dimension 1, may hold values from -3 to 3
- state_x: bfloat16 [2, 128, 3, 4096], P(None, ('grp', 'dp'), None, 'tp'), parts along dimension 1, may hold values from -6 to 6
- state_b: bfloat16 [2, 128, 3, 1024], P(None, ('grp', 'dp'), None, 'tp'), parts along dimension 1, may hold values from -6 to 6
- state_c: bfloat16 [2, 128, 3, 1024], P(None, ('grp', 'dp'), None, 'tp'), parts along dimension 1, may hold values from -6 to 6
Outputs:
- residual: bfloat16 [128, 2048], P(('grp', 'tp'), 'dp'), parts along dimension 0
- ssm_next: float32 [2, 128, 64, 64, 64], P(None, ('grp', 'dp'), 'tp'), parts along dimension 1
- next_x: bfloat16 [2, 128, 3, 4096], P(None, ('grp', 'dp'), None, 'tp'), parts along dimension 1
- next_b: bfloat16 [2, 128, 3, 1024], P(None, ('grp', 'dp'), None, 'tp'), parts along dimension 1
- next_c: bfloat16 [2, 128, 3, 1024], P(None, ('grp', 'dp'), None, 'tp'), parts along dimension 1
The draws below stay inside these ranges and needn't reach their ends.
There are 2 independent parts, one for each index of `grp`. The reference program is written for one: setup_inputs(seed, part) draws one part's arguments, and reference() takes and returns one part's arrays. A program takes and returns all parts, laid end to end along the dimension named above; an argument that names none is the same for every part. Nothing has to cross between parts.
All inputs are finite; a program needn't handle non-finite values.
Results may differ from the reference program's by a relative error of at most 0.0095.
Values may be sent and summed in bfloat16 or wider, within the bound.
A program may use at most 128 MiB of HBM per device.

```python
import jax
import jax.numpy as jnp
from jax import lax

D = 2048
HEADS = 64
HEAD_DIM = 64
GROUPS = 16
STATE = 64
KW = 4
LAYERS = 2
SW = 4096
SEQS = 64


def draw_tokens(key, part):
    ramp = jnp.exp(jnp.log(4.0) * jnp.arange(D, dtype=jnp.float32) / D)
    values = jnp.clip(jax.random.normal(jax.random.fold_in(key, 13), (SEQS, D), jnp.float32), -5.0, 5.0)
    return (values * ramp[None, :]).astype(jnp.bfloat16)


def block_levels(key, shape, cuts, low, high):
    level = 1.0
    for axis_at, blocks in cuts:
        steps = jax.random.uniform(jax.random.fold_in(jax.random.fold_in(key, 6), axis_at), (blocks,), jnp.float32, low / len(cuts), high / len(cuts))
        level = level * jnp.repeat(jnp.exp(steps), shape[axis_at] // blocks).reshape((-1,) + (1,) * (len(shape) - 1 - axis_at))
    return level


def normal_values(rng, dims, spread, most, split=(), kind=jnp.bfloat16):
    level = block_levels(rng, dims, split, -0.22, 0.18) if split else 1.0
    drawn = jax.random.normal(rng, dims, jnp.float32) * spread * level
    return jnp.minimum(jnp.maximum(drawn, -most), most).astype(kind)


def setup_inputs(seed: int = 0, part: int = 0) -> dict:
    arg_keys = jax.random.split(jax.random.key(seed), 20)
    part_splits = jax.random.split(jax.random.fold_in(arg_keys[19], part), 20)
    tokens = draw_tokens(jax.random.fold_in(jax.random.fold_in(arg_keys[19], part), 71), part)
    norm_gain = jnp.clip(1.0 + 0.18 * jax.random.normal(arg_keys[1], (LAYERS, D), jnp.float32), 0.099609375, 1.8984375).astype(jnp.bfloat16)
    w_z = normal_values(arg_keys[2], (LAYERS, D, SW), D ** -0.5, 0.125, ((1, 4), (2, 4)))
    w_x = normal_values(arg_keys[3], (LAYERS, D, SW), D ** -0.5, 0.125, ((1, 4), (2, 4)))
    w_b = normal_values(arg_keys[4], (LAYERS, D, GROUPS * STATE), D ** -0.5, 0.125, ((1, 4), (2, 4)))
    w_c = normal_values(arg_keys[5], (LAYERS, D, GROUPS * STATE), D ** -0.5, 0.125, ((1, 4), (2, 4)))
    w_dt = normal_values(arg_keys[6], (LAYERS, D, HEADS), D ** -0.5, 0.125, ((1, 4),))
    conv_x = normal_values(arg_keys[7], (LAYERS, KW, SW), 0.5, 3.0, ((2, 4),))
    conv_b = normal_values(arg_keys[8], (LAYERS, KW, GROUPS * STATE), 0.5, 3.0, ((2, 4),))
    conv_c = normal_values(arg_keys[9], (LAYERS, KW, GROUPS * STATE), 0.5, 3.0, ((2, 4),))
    dt_bias = jnp.clip(-3.0 + 3.5 * jax.random.uniform(arg_keys[10], (LAYERS, HEADS), jnp.float32) ** block_levels(arg_keys[10], (LAYERS, HEADS), ((1, 4),), -0.2, 0.2), -3.0, 0.5)
    a_log = jnp.clip(2.5 * jax.random.uniform(arg_keys[11], (LAYERS, HEADS), jnp.float32) ** block_levels(arg_keys[11], (LAYERS, HEADS), ((1, 4),), -0.2, 0.2), 0.0, 2.5)
    d_skip = jnp.clip(0.5 + 1.5 * jax.random.uniform(arg_keys[12], (LAYERS, HEADS), jnp.float32) ** block_levels(arg_keys[12], (LAYERS, HEADS), ((1, 4),), -0.2, 0.2), 0.5, 2.0)
    out_gain = jnp.clip(1.0 + 0.18 * jax.random.normal(arg_keys[13], (LAYERS, SW), jnp.float32), 0.099609375, 1.8984375).astype(jnp.bfloat16)
    w_out = normal_values(arg_keys[14], (LAYERS, SW, D), SW ** -0.5, 0.09375, ((1, 4), (2, 4)))
    ssm_state = normal_values(part_splits[15], (LAYERS, SEQS, HEADS, HEAD_DIM, STATE), 0.5, 3.0, ((1, 4), (2, 4)), jnp.float32)
    state_x = normal_values(part_splits[16], (LAYERS, SEQS, KW - 1, SW), 1.0, 6.0, ((1, 4), (3, 4)))
    state_b = normal_values(part_splits[17], (LAYERS, SEQS, KW - 1, GROUPS * STATE), 1.0, 6.0, ((1, 4), (3, 4)))
    state_c = normal_values(part_splits[18], (LAYERS, SEQS, KW - 1, GROUPS * STATE), 1.0, 6.0, ((1, 4), (3, 4)))
    return {"tokens": tokens, "norm_gain": norm_gain, "w_z": w_z, "w_x": w_x, "w_b": w_b, "w_c": w_c, "w_dt": w_dt, "conv_x": conv_x, "conv_b": conv_b, "conv_c": conv_c, "dt_bias": dt_bias, "a_log": a_log, "d_skip": d_skip, "out_gain": out_gain, "w_out": w_out, "ssm_state": ssm_state, "state_x": state_x, "state_b": state_b, "state_c": state_c}


EPSILON = 1e-05

def convolve(history, latest, weight):
    window = jnp.concatenate([history, latest[:, None, :]], axis=1)
    summed = lax.optimization_barrier(jnp.sum(window.astype(jnp.float32) * weight.astype(jnp.float32)[None], axis=1))
    return (jax.nn.silu(summed), window[:, 1:])

def mixer(gate_in, conv_xv, conv_bv, conv_cv, step_raw, bias, log_rate, skip, gain, state_prev):
    seq_count = conv_xv.shape[0]
    heads_here = step_raw.shape[1]
    group_count = conv_bv.shape[1] // STATE
    per_group = heads_here // group_count
    step_size = jax.nn.softplus(step_raw + bias)
    decay_rate = jnp.exp(-step_size * jnp.exp(log_rate))
    x_heads = conv_xv.reshape(seq_count, group_count, per_group, HEAD_DIM)
    b_state = conv_bv.reshape(seq_count, group_count, 1, 1, STATE)
    c_state = conv_cv.reshape(seq_count, group_count, 1, 1, STATE)
    step_heads = step_size.reshape(seq_count, group_count, per_group, 1)
    decay_heads = decay_rate.reshape(seq_count, group_count, per_group, 1, 1)
    previous = state_prev.reshape(seq_count, group_count, per_group, HEAD_DIM, STATE)
    state_next = decay_heads * previous + (step_heads * x_heads)[..., None] * b_state
    readout = lax.optimization_barrier(jnp.sum(state_next * c_state, axis=-1)) + skip.reshape(1, group_count, per_group, 1) * x_heads
    gated_out = readout.reshape(seq_count, group_count, -1) * jax.nn.silu(gate_in.astype(jnp.float32)).reshape(seq_count, group_count, -1)
    normed = gated_out * lax.rsqrt(lax.optimization_barrier(jnp.mean(gated_out * gated_out, axis=-1, keepdims=True)) + EPSILON)
    mixed_out = (normed.reshape(seq_count, -1) * gain.astype(jnp.float32)).astype(jnp.bfloat16)
    return (mixed_out, state_next.reshape(seq_count, heads_here, HEAD_DIM, STATE))

def reference(tokens, norm_gain, w_z, w_x, w_b, w_c, w_dt, conv_x, conv_b, conv_c, dt_bias, a_log, d_skip, out_gain, w_out, ssm_state, state_x, state_b, state_c):
    residual = tokens
    states, saved_x, saved_b, saved_c = ([], [], [], [])
    for layer_index in range(LAYERS):
        widened = residual.astype(jnp.float32)
        row_scale = lax.rsqrt(lax.optimization_barrier(jnp.mean(widened * widened, axis=1, keepdims=True)) + EPSILON)
        scaled = (widened * norm_gain[layer_index].astype(jnp.float32)).astype(jnp.bfloat16)
        gate_in = (jnp.dot(scaled, w_z[layer_index], preferred_element_type=jnp.float32) * row_scale).astype(jnp.bfloat16)
        x_in = (jnp.dot(scaled, w_x[layer_index], preferred_element_type=jnp.float32) * row_scale).astype(jnp.bfloat16)
        b_in = (jnp.dot(scaled, w_b[layer_index], preferred_element_type=jnp.float32) * row_scale).astype(jnp.bfloat16)
        c_in = (jnp.dot(scaled, w_c[layer_index], preferred_element_type=jnp.float32) * row_scale).astype(jnp.bfloat16)
        step_raw = jnp.dot(scaled, w_dt[layer_index], preferred_element_type=jnp.float32) * row_scale
        conv_xv, kept_x = convolve(state_x[layer_index], x_in, conv_x[layer_index])
        conv_bv, kept_b = convolve(state_b[layer_index], b_in, conv_b[layer_index])
        conv_cv, kept_c = convolve(state_c[layer_index], c_in, conv_c[layer_index])
        mixed_out, state_next = mixer(gate_in, conv_xv, conv_bv, conv_cv, step_raw, dt_bias[layer_index], a_log[layer_index], d_skip[layer_index], out_gain[layer_index], ssm_state[layer_index])
        projected = jnp.dot(mixed_out, w_out[layer_index], preferred_element_type=jnp.float32)
        residual = (widened + projected).astype(jnp.bfloat16)
        states.append(state_next)
        saved_x.append(kept_x)
        saved_b.append(kept_b)
        saved_c.append(kept_c)
    return (residual, jnp.stack(states), jnp.stack(saved_x), jnp.stack(saved_b), jnp.stack(saved_c))
```

```python
import functools

import jax
import jax.numpy as jnp
from jax import lax
from jax.experimental import pallas as pl
from jax.experimental.pallas import tpu as pltpu
from jax.sharding import PartitionSpec as P

HEAD_DIM = 64
STATE = 64
LANES = 128
EPSILON = 1e-05
MESH = pl.DeviceIdType.MESH
HBM = pl.BlockSpec(memory_space=pl.ANY)
VMEM = pl.BlockSpec(memory_space=pltpu.VMEM)


def padded(width):
    return -(-width // LANES) * LANES


def enter(sizes):
    barrier = pltpu.get_barrier_semaphore()
    count = 0
    for axis, size in sizes:
        me = lax.axis_index(axis)
        for k in range(1, size):
            pl.semaphore_signal(
                barrier, inc=1, device_id={axis: lax.rem(me + k, size)}, device_id_type=MESH
            )
            count += 1
    pl.semaphore_wait(barrier, count)


def push(axis, size, k, source, target, sems):
    me = lax.axis_index(axis)
    send, recv = sems
    return pltpu.make_async_remote_copy(
        src_ref=source,
        dst_ref=target,
        send_sem=send,
        recv_sem=recv,
        device_id={axis: lax.rem(me + k, size)},
        device_id_type=MESH,
    )


def start_loads(layer, pairs, sems):
    loads = []
    for i, (source, target) in enumerate(pairs):
        load = pltpu.make_async_copy(source.at[layer], target, sems.at[i])
        load.start()
        loads.append(load)
    return loads


def front(dims, layer, rows_ref, gain_ref, loads, scratch, outs):
    tp, dp, features = dims
    (wz, wx, wb, wc, wdt, gathered, total, half, got, side, side_got, sems) = scratch
    (ag_s, ag_r, rs_s, rs_r) = sems
    act_ref, step_ref = outs
    me_tp, me_dp = lax.axis_index("tp"), lax.axis_index("dp")
    rows, block = rows_ref.shape
    seqs = tp * rows // dp
    copies = []
    for k in range(1, tp):
        copy = push("tp", tp, k, rows_ref, gathered.at[me_tp], (ag_s.at[k], ag_r.at[k]))
        copy.start()
        copies.append(copy)
    gathered[me_tp] = rows_ref[...]
    for copy in copies:
        copy.wait()
    widened = gathered[...].reshape(tp * rows, block).astype(jnp.float32)
    scaled = (widened * gain_ref[layer : layer + 1, :].astype(jnp.float32)).astype(jnp.bfloat16)
    squares = jnp.sum(widened * widened, axis=1, keepdims=True)
    width, state_width, dt_width = wx.shape[1], wb.shape[1], wdt.shape[0]
    state_pad = padded(state_width)

    for load in loads:
        load.wait()
    dt = lax.dot_general(
        scaled, wdt[...], (((1,), (1,)), ((), ())), preferred_element_type=jnp.float32
    )
    side[...] = jnp.broadcast_to(squares, (dp * seqs, side.shape[2])).reshape(side.shape)
    side[:, :, 0:dt_width] = dt.reshape(dp, seqs, dt_width)
    copies = []
    for k in range(1, dp):
        peer = lax.rem(me_dp + k, dp)
        copy = push(
            "dp", dp, k, side.at[peer], side_got.at[k - 1], (rs_s.at[0, k], rs_r.at[0, k])
        )
        copy.start()
        copies.append(copy)
    spans = ((0, 0, wz, width), (1, 0, wx, width), (1, width, wb, state_width))
    spans = spans + ((1, width + state_pad, wc, state_width),)
    offsets = (0, width)
    for index, (piece, at, weight, size) in enumerate(spans):
        term = jnp.dot(scaled, weight[...], preferred_element_type=jnp.float32)
        term = term.reshape(dp, seqs, size)
        base = offsets[piece] + at
        total[:, :, base : base + size] = term
        half[piece][:, :, at : at + size] = term.astype(jnp.bfloat16)
        if index in (0, len(spans) - 1):
            for k in range(1, dp):
                peer = lax.rem(me_dp + k, dp)
                copy = push(
                    "dp",
                    dp,
                    k,
                    half[piece].at[peer],
                    got[piece].at[k - 1],
                    (rs_s.at[1 + piece, k], rs_r.at[1 + piece, k]),
                )
                copy.start()
                copies.append(copy)
    for copy in copies[: dp - 1]:
        copy.wait()
    side_sum = side[me_dp]
    for k in range(1, dp):
        side_sum = side_sum + side_got[k - 1]
    row_scale = lax.rsqrt(side_sum[:, LANES : LANES + 1] / features + EPSILON)
    step_ref[...] = side_sum[:, 0:LANES] * row_scale
    edges = (0, width, total.shape[2])
    for piece in range(2):
        for copy in copies[(piece + 1) * (dp - 1) : (piece + 2) * (dp - 1)]:
            copy.wait()
        value = total[me_dp, :, edges[piece] : edges[piece + 1]]
        for k in range(1, dp):
            value = value + got[piece][k - 1].astype(jnp.float32)
        act_ref[:, edges[piece] : edges[piece + 1]] = (value * row_scale).astype(jnp.bfloat16)


def back(dims, mixed_ref, rows_ref, load, scratch, out_ref):
    tp, dp, _ = dims
    wo, gathered, total, half, got, sems = scratch
    ag_s, ag_r, rs_s, rs_r = sems
    me_tp, me_dp = lax.axis_index("tp"), lax.axis_index("dp")
    seqs, width = mixed_ref.shape
    rows, block = rows_ref.shape
    copies = []
    for k in range(1, dp):
        copy = push("dp", dp, k, mixed_ref, gathered.at[me_dp], (ag_s.at[k], ag_r.at[k]))
        copy.start()
        copies.append(copy)
    gathered[me_dp] = mixed_ref[...]
    for copy in copies:
        copy.wait()
    load.wait()
    term = jnp.dot(
        gathered[...].reshape(dp * seqs, width), wo[...], preferred_element_type=jnp.float32
    ).reshape(tp, rows, block)
    total[...] = term
    half[...] = term.astype(jnp.bfloat16)
    copies = []
    for k in range(1, tp):
        peer = lax.rem(me_tp + k, tp)
        copy = push("tp", tp, k, half.at[peer], got.at[k - 1], (rs_s.at[k], rs_r.at[k]))
        copy.start()
        copies.append(copy)
    value = total[me_tp]
    for copy in copies:
        copy.wait()
    for k in range(1, tp):
        value = value + got[k - 1].astype(jnp.float32)
    out_ref[...] = (rows_ref[...].astype(jnp.float32) + value).astype(jnp.bfloat16)


def front_scratch(dims, rows, block, w_x, w_b, dt_width):
    tp, dp, _ = dims
    seqs = tp * rows // dp
    width, state = w_x.shape[2], w_b.shape[2]
    both = width + 2 * padded(state)
    bf, f32, dma = jnp.bfloat16, jnp.float32, pltpu.SemaphoreType.DMA
    weights = [
        pltpu.VMEM((block, width), bf),
        pltpu.VMEM((block, width), bf),
        pltpu.VMEM((block, state), bf),
        pltpu.VMEM((block, state), bf),
        pltpu.VMEM((dt_width, block), bf),
    ]
    rest = [
        pltpu.VMEM((tp, rows, block), bf),
        pltpu.VMEM((dp, seqs, width + both), f32),
        pltpu.VMEM((dp, seqs, width), bf),
        pltpu.VMEM((dp, seqs, both), bf),
        pltpu.VMEM((dp - 1, seqs, width), bf),
        pltpu.VMEM((dp - 1, seqs, both), bf),
        pltpu.VMEM((dp, seqs, 2 * LANES), f32),
        pltpu.VMEM((dp - 1, seqs, 2 * LANES), f32),
        dma((tp,)),
        dma((tp,)),
        dma((3, dp)),
        dma((3, dp)),
        dma((5,)),
    ]
    return weights + rest


def back_scratch(dims, rows, block, width):
    tp, dp, _ = dims
    seqs = tp * rows // dp
    bf, f32, dma = jnp.bfloat16, jnp.float32, pltpu.SemaphoreType.DMA
    return [
        pltpu.VMEM((width, block), bf),
        pltpu.VMEM((dp, seqs, width), bf),
        pltpu.VMEM((tp, rows, block), f32),
        pltpu.VMEM((tp, rows, block), bf),
        pltpu.VMEM((tp - 1, rows, block), bf),
        dma((dp,)),
        dma((dp,)),
        dma((tp,)),
        dma((tp,)),
        dma((1,)),
    ]


FRONT = 18
BACK = 10


def split_front(refs):
    wz, wx, wb, wc, wdt, gathered, total, h0, h1, g0, g1, side, side_got = refs[:13]
    scratch = (wz, wx, wb, wc, wdt, gathered, total, (h0, h1), (g0, g1), side, side_got)
    return scratch + (refs[13:17],), refs[17]


def kernel(dims, layer, has_back, has_front, *refs):
    tp, dp, _ = dims
    refs = list(refs)
    take = lambda n: [refs.pop(0) for _ in range(n)]
    rows_ref = take(1)[0]
    if has_back:
        mixed_ref, wo_ref = take(2)
    if has_front:
        gain_ref, *weights = take(6)
    new_ref = take(1)[0] if has_back else rows_ref
    outs = take(2) if has_front else None
    back_refs = take(BACK) if has_back else None
    front_refs = take(FRONT) if has_front else None
    if has_back:
        load = pltpu.make_async_copy(wo_ref.at[layer], back_refs[0], back_refs[-1].at[0])
        load.start()
    if has_front:
        scratch, load_sems = split_front(front_refs)
        here = layer + 1 if has_back else layer
        loads = start_loads(here, list(zip(weights, scratch[:5])), load_sems)
    enter((("tp", tp), ("dp", dp)))
    if has_back:
        pieces = tuple(back_refs[:5]) + (back_refs[5:9],)
        back(dims, mixed_ref, rows_ref, load, pieces, new_ref)
    if has_front:
        front(dims, here, new_ref, gain_ref, loads, scratch, outs)


def exchange(dims, number, layer, rows, mixed, w_out, norm_gain, weights):
    has_back, has_front = mixed is not None, weights is not None
    tp, dp, _ = dims
    count, block = rows.shape
    seqs = tp * count // dp
    operands, specs, shapes, scratch = [rows], [VMEM], [], []
    if has_back:
        operands += [mixed, w_out]
        specs += [VMEM, HBM]
        shapes.append(jax.ShapeDtypeStruct(rows.shape, jnp.bfloat16))
        scratch += back_scratch(dims, count, block, mixed.shape[1])
    if has_front:
        operands += [norm_gain, *weights]
        specs += [VMEM] + [HBM] * 5
        w_x, w_b, w_dt = weights[1], weights[2], weights[4]
        across = 2 * w_x.shape[2] + 2 * padded(w_b.shape[2])
        shapes.append(jax.ShapeDtypeStruct((seqs, across), jnp.bfloat16))
        shapes.append(jax.ShapeDtypeStruct((seqs, LANES), jnp.float32))
        scratch += front_scratch(dims, count, block, w_x, w_b, w_dt.shape[1])
    return pl.pallas_call(
        functools.partial(kernel, dims, layer, has_back, has_front),
        out_shape=shapes,
        in_specs=specs,
        out_specs=[VMEM] * len(shapes),
        scratch_shapes=scratch,
        compiler_params=pltpu.CompilerParams(
            collective_id=number, has_side_effects=True, vmem_limit_bytes=40 * 2**20
        ),
    )(*operands)


def convolve(history, latest, weight):
    window = jnp.concatenate([history, latest[:, None, :]], axis=1)
    summed = jnp.sum(window.astype(jnp.float32) * weight.astype(jnp.float32)[None], axis=1)
    return (jax.nn.silu(summed), window[:, 1:])


def mixer(gate_in, conv_xv, conv_bv, conv_cv, step_raw, bias, log_rate, skip, gain, state_prev):
    seq_count = conv_xv.shape[0]
    heads_here = step_raw.shape[1]
    group_count = conv_bv.shape[1] // STATE
    per_group = heads_here // group_count
    step_size = jax.nn.softplus(step_raw + bias)
    decay_rate = jnp.exp(-step_size * jnp.exp(log_rate))
    x_heads = conv_xv.reshape(seq_count, group_count, per_group, HEAD_DIM)
    b_state = conv_bv.reshape(seq_count, group_count, 1, 1, STATE)
    c_state = conv_cv.reshape(seq_count, group_count, 1, 1, STATE)
    step_heads = step_size.reshape(seq_count, group_count, per_group, 1)
    decay_heads = decay_rate.reshape(seq_count, group_count, per_group, 1, 1)
    previous = state_prev.reshape(seq_count, group_count, per_group, HEAD_DIM, STATE)
    state_next = decay_heads * previous + (step_heads * x_heads)[..., None] * b_state
    readout = (
        jnp.sum(state_next * c_state, axis=-1)
        + skip.reshape(1, group_count, per_group, 1) * x_heads
    )
    gated_out = readout.reshape(seq_count, group_count, -1) * jax.nn.silu(
        gate_in.astype(jnp.float32)
    ).reshape(seq_count, group_count, -1)
    normed = gated_out * lax.rsqrt(
        jnp.mean(gated_out * gated_out, axis=-1, keepdims=True) + EPSILON
    )
    mixed_out = (normed.reshape(seq_count, -1) * gain.astype(jnp.float32)).astype(jnp.bfloat16)
    factors = (decay_heads[..., 0, 0], step_heads * x_heads, b_state[:, :, 0, 0, :])
    return mixed_out, factors


def body(
    tokens,
    norm_gain,
    w_z,
    w_x,
    w_b,
    w_c,
    w_dt,
    conv_x,
    conv_b,
    conv_c,
    dt_bias,
    a_log,
    d_skip,
    out_gain,
    w_out,
    ssm_state,
    state_x,
    state_b,
    state_c,
):
    tp, dp = lax.axis_size("tp"), lax.axis_size("dp")
    dims = (tp, dp, tokens.shape[1] * dp)
    weights = (w_z, w_x, w_b, w_c, jnp.swapaxes(w_dt, 1, 2))
    layers = w_z.shape[0]
    width, state_width = w_x.shape[2], w_b.shape[2]
    state_pad = padded(state_width)
    heads_here = dt_bias.shape[1]
    residual = tokens
    act, steps = exchange(dims, 0, 0, residual, None, None, norm_gain, weights)
    kept, factors = [], []
    for layer in range(layers):
        gate_in = act[:, 0:width]
        x_in = act[:, width : 2 * width]
        b_in = act[:, 2 * width : 2 * width + state_width]
        c_in = act[:, 2 * width + state_pad : 2 * width + state_pad + state_width]
        step_raw = lax.dynamic_slice_in_dim(steps, lax.axis_index("tp") * heads_here, heads_here, 1)
        conv_xv, kept_x = convolve(state_x[layer], x_in, conv_x[layer])
        conv_bv, kept_b = convolve(state_b[layer], b_in, conv_b[layer])
        conv_cv, kept_c = convolve(state_c[layer], c_in, conv_c[layer])
        mixed, pieces = mixer(
            gate_in,
            conv_xv,
            conv_bv,
            conv_cv,
            step_raw,
            dt_bias[layer],
            a_log[layer],
            d_skip[layer],
            out_gain[layer],
            ssm_state[layer],
        )
        kept.append((kept_x, kept_b, kept_c))
        factors.append(pieces)
        if layer + 1 < layers:
            residual, act, steps = exchange(
                dims, layer + 1, layer, residual, mixed, w_out, norm_gain, weights
            )
        else:
            (residual,) = exchange(dims, layer + 1, layer, residual, mixed, w_out, None, None)
    decay, added, inputs = (jnp.stack(each) for each in zip(*factors))
    decay, added, inputs = lax.optimization_barrier((decay, added, inputs))
    previous = ssm_state.reshape(decay.shape + (HEAD_DIM, STATE))
    state_next = decay[..., None, None] * previous + added[..., None] * inputs[:, :, :, None, None]
    saved = (jnp.stack(each) for each in zip(*kept))
    return (residual, state_next.reshape(ssm_state.shape), *saved)


def solution(mesh):
    placed = (
        P(("grp", "tp"), "dp"),
        P(None, "dp"),
        P(None, "dp", "tp"),
        P(None, "dp", "tp"),
        P(None, "dp", "tp"),
        P(None, "dp", "tp"),
        P(None, "dp", None),
        P(None, None, "tp"),
        P(None, None, "tp"),
        P(None, None, "tp"),
        P(None, "tp"),
        P(None, "tp"),
        P(None, "tp"),
        P(None, "tp"),
        P(None, "tp", "dp"),
        P(None, ("grp", "dp"), "tp", None, None),
        P(None, ("grp", "dp"), None, "tp"),
        P(None, ("grp", "dp"), None, "tp"),
        P(None, ("grp", "dp"), None, "tp"),
    )
    return jax.shard_map(
        body,
        mesh=mesh,
        in_specs=placed,
        out_specs=(
            P(("grp", "tp"), "dp"),
            P(None, ("grp", "dp"), "tp", None, None),
            P(None, ("grp", "dp"), None, "tp"),
            P(None, ("grp", "dp"), None, "tp"),
            P(None, ("grp", "dp"), None, "tp"),
        ),
        check_vma=False,
    )
```

```python
import functools

import jax
import jax.numpy as jnp
from jax import lax
from jax.experimental import pallas as pl
from jax.experimental.pallas import tpu as pltpu
from jax.sharding import PartitionSpec as P

HEAD_DIM = 64
STATE = 64
LANES = 128
EPSILON = 1e-05
MESH = pl.DeviceIdType.MESH
HBM = pl.BlockSpec(memory_space=pltpu.HBM)
VMEM = pl.BlockSpec(memory_space=pltpu.VMEM)


def padded(width):
    return -(-width // LANES) * LANES


def enter(sizes):
    barrier = pltpu.get_barrier_semaphore()
    count = 0
    for axis, size in sizes:
        me = lax.axis_index(axis)
        for k in range(1, size):
            pl.semaphore_signal(
                barrier, inc=1, device_id={axis: lax.rem(me + k, size)}, device_id_type=MESH
            )
            count += 1
    pl.semaphore_wait(barrier, count)


def push(axis, size, k, source, target, sems):
    me = lax.axis_index(axis)
    send, recv = sems
    return pltpu.make_async_remote_copy(
        src_ref=source,
        dst_ref=target,
        send_sem=send,
        recv_sem=recv,
        device_id={axis: lax.rem(me + k, size)},
        device_id_type=MESH,
    )


def start_loads(layer, pairs, sems):
    loads = []
    for i, (source, target) in enumerate(pairs):
        load = pltpu.make_async_copy(source.at[layer], target, sems.at[i])
        load.start()
        loads.append(load)
    return loads


def front(dims, layer, rows_ref, gain_ref, loads, scratch, outs):
    tp, dp, features = dims
    (wz, wx, wb, wc, wdt, gathered, total, half, got, side, side_got, sems) = scratch
    (ag_s, ag_r, rs_s, rs_r) = sems
    act_ref, step_ref = outs
    me_tp, me_dp = lax.axis_index("tp"), lax.axis_index("dp")
    rows, block = rows_ref.shape
    seqs = tp * rows // dp
    copies = []
    for k in range(1, tp):
        copy = push("tp", tp, k, rows_ref, gathered.at[me_tp], (ag_s.at[k], ag_r.at[k]))
        copy.start()
        copies.append(copy)
    gathered[me_tp] = rows_ref[...]
    for copy in copies:
        copy.wait()
    widened = gathered[...].reshape(tp * rows, block).astype(jnp.float32)
    scaled = (widened * gain_ref[layer : layer + 1, :].astype(jnp.float32)).astype(jnp.bfloat16)
    squares = jnp.sum(widened * widened, axis=1, keepdims=True)
    width, state_width, dt_width = wx.shape[1], wb.shape[1], wdt.shape[0]
    state_pad = padded(state_width)

    for load in loads:
        load.wait()
    dt = lax.dot_general(
        scaled, wdt[...], (((1,), (1,)), ((), ())), preferred_element_type=jnp.float32
    )
    side[...] = jnp.broadcast_to(squares, (dp * seqs, side.shape[2])).reshape(side.shape)
    side[:, :, 0:dt_width] = dt.reshape(dp, seqs, dt_width)
    copies = []
    for k in range(1, dp):
        peer = lax.rem(me_dp + k, dp)
        copy = push(
            "dp", dp, k, side.at[peer], side_got.at[k - 1], (rs_s.at[0, k], rs_r.at[0, k])
        )
        copy.start()
        copies.append(copy)
    spans = ((0, 0, wz, width), (1, 0, wx, width), (1, width, wb, state_width))
    spans = spans + ((1, width + state_pad, wc, state_width),)
    offsets = (0, width)
    for index, (piece, at, weight, size) in enumerate(spans):
        term = jnp.dot(scaled, weight[...], preferred_element_type=jnp.float32)
        term = term.reshape(dp, seqs, size)
        base = offsets[piece] + at
        total[:, :, base : base + size] = term
        half[piece][:, :, at : at + size] = term.astype(jnp.bfloat16)
        if index in (0, len(spans) - 1):
            for k in range(1, dp):
                peer = lax.rem(me_dp + k, dp)
                copy = push(
                    "dp",
                    dp,
                    k,
                    half[piece].at[peer],
                    got[piece].at[k - 1],
                    (rs_s.at[1 + piece, k], rs_r.at[1 + piece, k]),
                )
                copy.start()
                copies.append(copy)
    for copy in copies[: dp - 1]:
        copy.wait()
    side_sum = side[me_dp]
    for k in range(1, dp):
        side_sum = side_sum + side_got[k - 1]
    row_scale = lax.rsqrt(side_sum[:, LANES : LANES + 1] / features + EPSILON)
    shift = lax.rem(LANES - me_tp * (dt_width // tp), LANES)
    step_ref[...] = pltpu.roll(side_sum[:, 0:LANES] * row_scale, shift, 1)
    edges = (0, width, total.shape[2])
    for piece in range(2):
        for copy in copies[(piece + 1) * (dp - 1) : (piece + 2) * (dp - 1)]:
            copy.wait()
        value = total[me_dp, :, edges[piece] : edges[piece + 1]]
        for k in range(1, dp):
            value = value + got[piece][k - 1].astype(jnp.float32)
        act_ref[:, edges[piece] : edges[piece + 1]] = (value * row_scale).astype(jnp.bfloat16)


def back(dims, mixed_ref, rows_ref, load, scratch, out_ref):
    tp, dp, _ = dims
    wo, gathered, total, half, got, sems = scratch
    ag_s, ag_r, rs_s, rs_r = sems
    me_tp, me_dp = lax.axis_index("tp"), lax.axis_index("dp")
    seqs, width = mixed_ref.shape
    rows, block = rows_ref.shape
    copies = []
    for k in range(1, dp):
        copy = push("dp", dp, k, mixed_ref, gathered.at[me_dp], (ag_s.at[k], ag_r.at[k]))
        copy.start()
        copies.append(copy)
    gathered[me_dp] = mixed_ref[...]
    for copy in copies:
        copy.wait()
    load.wait()
    term = jnp.dot(
        gathered[...].reshape(dp * seqs, width), wo[...], preferred_element_type=jnp.float32
    ).reshape(tp, rows, block)
    total[...] = term
    half[...] = term.astype(jnp.bfloat16)
    copies = []
    for k in range(1, tp):
        peer = lax.rem(me_tp + k, tp)
        copy = push("tp", tp, k, half.at[peer], got.at[k - 1], (rs_s.at[k], rs_r.at[k]))
        copy.start()
        copies.append(copy)
    value = total[me_tp]
    for copy in copies:
        copy.wait()
    for k in range(1, tp):
        value = value + got[k - 1].astype(jnp.float32)
    out_ref[...] = (rows_ref[...].astype(jnp.float32) + value).astype(jnp.bfloat16)


def front_scratch(dims, rows, block, w_x, w_b, dt_width):
    tp, dp, _ = dims
    seqs = tp * rows // dp
    width, state = w_x.shape[2], w_b.shape[2]
    both = width + 2 * padded(state)
    bf, f32, dma = jnp.bfloat16, jnp.float32, pltpu.SemaphoreType.DMA
    weights = [
        pltpu.VMEM((block, width), bf),
        pltpu.VMEM((block, width), bf),
        pltpu.VMEM((block, state), bf),
        pltpu.VMEM((block, state), bf),
        pltpu.VMEM((dt_width, block), bf),
    ]
    rest = [
        pltpu.VMEM((tp, rows, block), bf),
        pltpu.VMEM((dp, seqs, width + both), f32),
        pltpu.VMEM((dp, seqs, width), bf),
        pltpu.VMEM((dp, seqs, both), bf),
        pltpu.VMEM((dp - 1, seqs, width), bf),
        pltpu.VMEM((dp - 1, seqs, both), bf),
        pltpu.VMEM((dp, seqs, 2 * LANES), f32),
        pltpu.VMEM((dp - 1, seqs, 2 * LANES), f32),
        dma((tp,)),
        dma((tp,)),
        dma((3, dp)),
        dma((3, dp)),
        dma((5,)),
    ]
    return weights + rest


def back_scratch(dims, rows, block, width):
    tp, dp, _ = dims
    seqs = tp * rows // dp
    bf, f32, dma = jnp.bfloat16, jnp.float32, pltpu.SemaphoreType.DMA
    return [
        pltpu.VMEM((width, block), bf),
        pltpu.VMEM((dp, seqs, width), bf),
        pltpu.VMEM((tp, rows, block), f32),
        pltpu.VMEM((tp, rows, block), bf),
        pltpu.VMEM((tp - 1, rows, block), bf),
        dma((dp,)),
        dma((dp,)),
        dma((tp,)),
        dma((tp,)),
        dma((1,)),
    ]


FRONT = 18
BACK = 10


def split_front(refs):
    wz, wx, wb, wc, wdt, gathered, total, h0, h1, g0, g1, side, side_got = refs[:13]
    scratch = (wz, wx, wb, wc, wdt, gathered, total, (h0, h1), (g0, g1), side, side_got)
    return scratch + (refs[13:17],), refs[17]


def kernel(dims, layer, has_back, has_front, *refs):
    tp, dp, _ = dims
    refs = list(refs)
    take = lambda n: [refs.pop(0) for _ in range(n)]
    rows_ref = take(1)[0]
    if has_back:
        mixed_ref, wo_ref = take(2)
    if has_front:
        gain_ref, *weights = take(6)
    new_ref = take(1)[0] if has_back else rows_ref
    outs = take(2) if has_front else None
    back_refs = take(BACK) if has_back else None
    front_refs = take(FRONT) if has_front else None
    if has_back:
        load = pltpu.make_async_copy(wo_ref.at[layer], back_refs[0], back_refs[-1].at[0])
        load.start()
    if has_front:
        scratch, load_sems = split_front(front_refs)
        here = layer + 1 if has_back else layer
        loads = start_loads(here, list(zip(weights, scratch[:5])), load_sems)
    enter((("tp", tp), ("dp", dp)))
    if has_back:
        pieces = tuple(back_refs[:5]) + (back_refs[5:9],)
        back(dims, mixed_ref, rows_ref, load, pieces, new_ref)
    if has_front:
        front(dims, here, new_ref, gain_ref, loads, scratch, outs)


def exchange(dims, number, layer, rows, mixed, w_out, norm_gain, weights):
    has_back, has_front = mixed is not None, weights is not None
    tp, dp, _ = dims
    count, block = rows.shape
    seqs = tp * count // dp
    operands, specs, shapes, scratch = [rows], [VMEM], [], []
    if has_back:
        operands += [mixed, w_out]
        specs += [VMEM, HBM]
        shapes.append(jax.ShapeDtypeStruct(rows.shape, jnp.bfloat16))
        scratch += back_scratch(dims, count, block, mixed.shape[1])
    if has_front:
        operands += [norm_gain, *weights]
        specs += [VMEM] + [HBM] * 5
        w_x, w_b, w_dt = weights[1], weights[2], weights[4]
        across = 2 * w_x.shape[2] + 2 * padded(w_b.shape[2])
        shapes.append(jax.ShapeDtypeStruct((seqs, across), jnp.bfloat16))
        shapes.append(jax.ShapeDtypeStruct((seqs, LANES), jnp.float32))
        scratch += front_scratch(dims, count, block, w_x, w_b, w_dt.shape[1])
    return pl.pallas_call(
        functools.partial(kernel, dims, layer, has_back, has_front),
        out_shape=shapes,
        in_specs=specs,
        out_specs=[VMEM] * len(shapes),
        scratch_shapes=scratch,
        compiler_params=pltpu.CompilerParams(
            collective_id=number, has_side_effects=True, vmem_limit_bytes=56 * 2**20
        ),
    )(*operands)


def convolve(history_ref, latest, taps_ref, layer, kept_ref):
    weight = taps_ref[layer].astype(jnp.float32)
    old = history_ref.shape[1]
    summed = latest.astype(jnp.float32) * weight[old : old + 1]
    for k in range(old):
        summed = summed + history_ref[0, k].astype(jnp.float32) * weight[k : k + 1]
    for k in range(1, old):
        kept_ref[0, k - 1] = history_ref[0, k]
    kept_ref[0, old - 1] = latest
    return summed * jax.nn.sigmoid(summed)


def mix_kernel(layer, heads_step, aliased, *refs):
    act, steps, tap_x, tap_b, tap_c, bias, rate, skip, gain, prev, old_x, old_b, old_c = refs[:13]
    mixed, state, kept_x, kept_b, kept_c = refs[13 + aliased : 18 + aliased]
    skipped, factors, b_rows, c_rows, read = refs[18 + aliased :]
    seqs, width = mixed.shape
    heads = bias.shape[1]
    groups = b_rows.shape[0]
    per_group = heads // groups
    state_width = kept_b.shape[3]
    at = pl.program_id(0)

    @pl.when(at == 0)
    def _():
        raw = steps[:, 0:heads] + bias[layer : layer + 1, :]
        size = jnp.maximum(raw, 0.0) + jnp.log1p(jnp.exp(-jnp.abs(raw)))
        decay = jnp.exp(-size * jnp.exp(rate[layer : layer + 1, :]))
        skips = jnp.broadcast_to(skip[layer : layer + 1, :], (8, heads))
        stacked = jnp.concatenate([size, decay, skips], axis=0)
        row = lax.broadcasted_iota(jnp.int32, (heads, width), 0)
        lane = lax.broadcasted_iota(jnp.int32, (heads, width), 1)
        first = row * HEAD_DIM
        spread = jnp.where((lane >= first) & (lane < first + HEAD_DIM), 1.0, 0.0)
        wide = jnp.dot(
            stacked, spread, precision=lax.Precision.HIGHEST, preferred_element_type=jnp.float32
        )
        conv = convolve(old_x, act[:, width : 2 * width], tap_x, layer, kept_x)
        skipped[...] = wide[2 * seqs : 2 * seqs + 1] * conv
        both = jnp.concatenate([wide[0:seqs] * conv, wide[seqs : 2 * seqs]], axis=0)
        factors[...] = both.T
        begin = 2 * width
        for target, old, tap, kept in ((b_rows, old_b, tap_b, kept_b), (c_rows, old_c, tap_c, kept_c)):
            conv = convolve(old, act[:, begin : begin + state_width], tap, layer, kept)
            for g in range(groups):
                target[g] = conv[:, g * STATE : (g + 1) * STATE]
            begin += padded(state_width)

    group = at * heads_step // per_group
    b_here, c_here = b_rows[group], c_rows[group]
    spot = lax.broadcasted_iota(jnp.int32, (HEAD_DIM, seqs), 1)
    for j in range(heads_step):
        first = pl.multiple_of((at * heads_step + j) * HEAD_DIM, HEAD_DIM)
        columns = factors[pl.ds(first, HEAD_DIM), :]
        taken = jnp.zeros((HEAD_DIM, seqs), jnp.float32)
        for s in range(seqs):
            fade = columns[:, seqs + s : seqs + s + 1]
            new = fade * prev[0, s, j] + columns[:, s : s + 1] * b_here[s : s + 1, :]
            state[0, s, j] = new
            summed = jnp.sum(new * c_here[s : s + 1, :], axis=1, keepdims=True)
            taken = jnp.where(spot == s, summed, taken)
        read[pl.ds(first, HEAD_DIM), :] = taken

    @pl.when(at == pl.num_programs(0) - 1)
    def _():
        gate = act[:, 0:width].astype(jnp.float32)
        gated = (read[...].T + skipped[...]) * (gate * jax.nn.sigmoid(gate))
        span = per_group * HEAD_DIM
        for g in range(groups):
            part = gated[:, g * span : (g + 1) * span]
            scale = lax.rsqrt(jnp.mean(part * part, axis=1, keepdims=True) + EPSILON)
            gains = gain[layer : layer + 1, g * span : (g + 1) * span].astype(jnp.float32)
            mixed[:, g * span : (g + 1) * span] = (part * scale * gains).astype(jnp.bfloat16)


def mix(layer, act, steps, params, state, olds, carried):
    seqs, heads = state.shape[1:3]
    width, state_width = olds[0].shape[3], olds[1].shape[3]
    groups = state_width // STATE
    per_group = heads // groups
    heads_step = 2 if per_group % 2 == 0 else 1
    seqs_dim = lambda ref: (1,) + ref.shape[1:]
    whole = lambda ref: pl.BlockSpec(ref.shape, lambda i, n=ref.ndim: (0,) * n)
    at_layer = lambda ref: pl.BlockSpec(seqs_dim(ref), lambda i, n=ref.ndim: (layer,) + (0,) * (n - 1))
    tile = pl.BlockSpec(
        (1, seqs, heads_step, HEAD_DIM, STATE), lambda i: (layer, 0, i, 0, 0)
    )
    operands = [act, steps, *params, state, *olds]
    specs = [whole(x) for x in (act, steps, *params)] + [tile] + [at_layer(x) for x in olds]
    aliases = {}
    if carried is not None:
        aliases = {len(operands) + i: 1 + i for i in range(4)}
        operands += carried
        specs += [pl.BlockSpec(memory_space=pl.ANY)] * 4
    kinds = [jax.ShapeDtypeStruct(x.shape, x.dtype) for x in (state, *olds)]
    mixed = jax.ShapeDtypeStruct((seqs, width), jnp.bfloat16)
    f32 = jnp.float32
    return pl.pallas_call(
        functools.partial(mix_kernel, layer, heads_step, len(aliases)),
        grid=(heads // heads_step,),
        out_shape=[mixed] + kinds,
        in_specs=specs,
        out_specs=[whole(mixed), tile] + [at_layer(x) for x in olds],
        scratch_shapes=[
            pltpu.VMEM((seqs, width), f32),
            pltpu.VMEM((width, 2 * seqs), f32),
            pltpu.VMEM((groups, seqs, STATE), f32),
            pltpu.VMEM((groups, seqs, STATE), f32),
            pltpu.VMEM((width, seqs), f32),
        ],
        input_output_aliases=aliases,
        compiler_params=pltpu.CompilerParams(
            dimension_semantics=("arbitrary",), vmem_limit_bytes=56 * 2**20
        ),
    )(*operands)


def body(
    tokens,
    norm_gain,
    w_z,
    w_x,
    w_b,
    w_c,
    w_dt,
    conv_x,
    conv_b,
    conv_c,
    dt_bias,
    a_log,
    d_skip,
    out_gain,
    w_out,
    ssm_state,
    state_x,
    state_b,
    state_c,
):
    tp, dp = lax.axis_size("tp"), lax.axis_size("dp")
    dims = (tp, dp, tokens.shape[1] * dp)
    weights = (w_z, w_x, w_b, w_c, jnp.swapaxes(w_dt, 1, 2))
    layers = w_z.shape[0]
    params = (conv_x, conv_b, conv_c, dt_bias, a_log, d_skip, out_gain)
    olds = [jnp.swapaxes(x, 1, 2) for x in (state_x, state_b, state_c)]
    residual = tokens
    act, steps = exchange(dims, 0, 0, residual, None, None, norm_gain, weights)
    carried = None
    for layer in range(layers):
        mixed, *carried = mix(layer, act, steps, params, ssm_state, olds, carried)
        if layer + 1 < layers:
            residual, act, steps = exchange(
                dims, layer + 1, layer, residual, mixed, w_out, norm_gain, weights
            )
        else:
            (residual,) = exchange(dims, layer + 1, layer, residual, mixed, w_out, None, None)
    return (residual, carried[0], *(jnp.swapaxes(x, 1, 2) for x in carried[1:]))


def solution(mesh):
    placed = (
        P(("grp", "tp"), "dp"),
        P(None, "dp"),
        P(None, "dp", "tp"),
        P(None, "dp", "tp"),
        P(None, "dp", "tp"),
        P(None, "dp", "tp"),
        P(None, "dp", None),
        P(None, None, "tp"),
        P(None, None, "tp"),
        P(None, None, "tp"),
        P(None, "tp"),
        P(None, "tp"),
        P(None, "tp"),
        P(None, "tp"),
        P(None, "tp", "dp"),
        P(None, ("grp", "dp"), "tp", None, None),
        P(None, ("grp", "dp"), None, "tp"),
        P(None, ("grp", "dp"), None, "tp"),
        P(None, ("grp", "dp"), None, "tp"),
    )
    return jax.shard_map(
        body,
        mesh=mesh,
        in_specs=placed,
        out_specs=(
            P(("grp", "tp"), "dp"),
            P(None, ("grp", "dp"), "tp", None, None),
            P(None, ("grp", "dp"), None, "tp"),
            P(None, ("grp", "dp"), None, "tp"),
            P(None, ("grp", "dp"), None, "tp"),
        ),
        check_vma=False,
    )
```

```python
import functools

import jax
import jax.numpy as jnp
from jax import lax
from jax.experimental import pallas as pl
from jax.experimental.pallas import tpu as pltpu
from jax.sharding import PartitionSpec as P

HEAD_DIM = 64
STATE = 64
LANES = 128
EPSILON = 1e-05
MESH = pl.DeviceIdType.MESH
HBM = pl.BlockSpec(memory_space=pltpu.HBM)
VMEM = pl.BlockSpec(memory_space=pltpu.VMEM)


def padded(width):
    return -(-width // LANES) * LANES


def enter(sizes):
    barrier = pltpu.get_barrier_semaphore()
    count = 0
    for axis, size in sizes:
        me = lax.axis_index(axis)
        for k in range(1, size):
            pl.semaphore_signal(
                barrier, inc=1, device_id={axis: lax.rem(me + k, size)}, device_id_type=MESH
            )
            count += 1
    pl.semaphore_wait(barrier, count)


def push(axis, size, k, source, target, sems):
    me = lax.axis_index(axis)
    send, recv = sems
    return pltpu.make_async_remote_copy(
        src_ref=source,
        dst_ref=target,
        send_sem=send,
        recv_sem=recv,
        device_id={axis: lax.rem(me + k, size)},
        device_id_type=MESH,
    )


def start_loads(layer, pairs, sems):
    loads = []
    for i, (source, target) in enumerate(pairs):
        load = pltpu.make_async_copy(source.at[layer], target, sems.at[i])
        load.start()
        loads.append(load)
    return loads


def front(dims, layer, rows_ref, gain_ref, loads, scratch, outs):
    tp, dp, features = dims
    (wz, wx, wb, wc, wdt, gathered, total, half, got, side, side_got, sems) = scratch
    (ag_s, ag_r, rs_s, rs_r) = sems
    act_ref, step_ref = outs
    me_tp, me_dp = lax.axis_index("tp"), lax.axis_index("dp")
    rows, block = rows_ref.shape
    seqs = tp * rows // dp
    copies = []
    for k in range(1, tp):
        copy = push("tp", tp, k, rows_ref, gathered.at[me_tp], (ag_s.at[k], ag_r.at[k]))
        copy.start()
        copies.append(copy)
    gathered[me_tp] = rows_ref[...]
    for copy in copies:
        copy.wait()
    widened = gathered[...].reshape(tp * rows, block).astype(jnp.float32)
    scaled = (widened * gain_ref[layer : layer + 1, :].astype(jnp.float32)).astype(jnp.bfloat16)
    squares = jnp.sum(widened * widened, axis=1, keepdims=True)
    width, state_width, dt_width = wx.shape[1], wb.shape[1], wdt.shape[0]
    state_pad = padded(state_width)

    for load in loads:
        load.wait()
    dt = lax.dot_general(
        scaled, wdt[...], (((1,), (1,)), ((), ())), preferred_element_type=jnp.float32
    )
    side[...] = jnp.broadcast_to(squares, (dp * seqs, side.shape[2])).reshape(side.shape)
    side[:, :, 0:dt_width] = dt.reshape(dp, seqs, dt_width)
    copies = []
    for k in range(1, dp):
        peer = lax.rem(me_dp + k, dp)
        copy = push(
            "dp", dp, k, side.at[peer], side_got.at[k - 1], (rs_s.at[0, k], rs_r.at[0, k])
        )
        copy.start()
        copies.append(copy)
    spans = ((0, 0, wz, width), (1, 0, wx, width), (1, width, wb, state_width))
    spans = spans + ((1, width + state_pad, wc, state_width),)
    offsets = (0, width)
    for index, (piece, at, weight, size) in enumerate(spans):
        term = jnp.dot(scaled, weight[...], preferred_element_type=jnp.float32)
        term = term.reshape(dp, seqs, size)
        base = offsets[piece] + at
        total[:, :, base : base + size] = term
        half[piece][:, :, at : at + size] = term.astype(jnp.bfloat16)
        if index in (0, len(spans) - 1):
            for k in range(1, dp):
                peer = lax.rem(me_dp + k, dp)
                copy = push(
                    "dp",
                    dp,
                    k,
                    half[piece].at[peer],
                    got[piece].at[k - 1],
                    (rs_s.at[1 + piece, k], rs_r.at[1 + piece, k]),
                )
                copy.start()
                copies.append(copy)
    for copy in copies[: dp - 1]:
        copy.wait()
    side_sum = side[me_dp]
    for k in range(1, dp):
        side_sum = side_sum + side_got[k - 1]
    row_scale = lax.rsqrt(side_sum[:, LANES : LANES + 1] / features + EPSILON)
    shift = lax.rem(LANES - me_tp * (dt_width // tp), LANES)
    step_ref[...] = pltpu.roll(side_sum[:, 0:LANES] * row_scale, shift, 1)
    edges = (0, width, total.shape[2])
    for piece in range(2):
        for copy in copies[(piece + 1) * (dp - 1) : (piece + 2) * (dp - 1)]:
            copy.wait()
        value = total[me_dp, :, edges[piece] : edges[piece + 1]]
        for k in range(1, dp):
            value = value + got[piece][k - 1].astype(jnp.float32)
        act_ref[:, edges[piece] : edges[piece + 1]] = (value * row_scale).astype(jnp.bfloat16)


def back(dims, mixed_ref, rows_ref, load, scratch, out_ref):
    tp, dp, _ = dims
    wo, gathered, total, half, got, sems = scratch
    ag_s, ag_r, rs_s, rs_r = sems
    me_tp, me_dp = lax.axis_index("tp"), lax.axis_index("dp")
    seqs, width = mixed_ref.shape
    rows, block = rows_ref.shape
    copies = []
    for k in range(1, dp):
        copy = push("dp", dp, k, mixed_ref, gathered.at[me_dp], (ag_s.at[k], ag_r.at[k]))
        copy.start()
        copies.append(copy)
    gathered[me_dp] = mixed_ref[...]
    for copy in copies:
        copy.wait()
    load.wait()
    term = jnp.dot(
        gathered[...].reshape(dp * seqs, width), wo[...], preferred_element_type=jnp.float32
    ).reshape(tp, rows, block)
    total[...] = term
    half[...] = term.astype(jnp.bfloat16)
    copies = []
    for k in range(1, tp):
        peer = lax.rem(me_tp + k, tp)
        copy = push("tp", tp, k, half.at[peer], got.at[k - 1], (rs_s.at[k], rs_r.at[k]))
        copy.start()
        copies.append(copy)
    value = total[me_tp]
    for copy in copies:
        copy.wait()
    for k in range(1, tp):
        value = value + got[k - 1].astype(jnp.float32)
    out_ref[...] = (rows_ref[...].astype(jnp.float32) + value).astype(jnp.bfloat16)


def front_scratch(dims, rows, block, w_x, w_b, dt_width):
    tp, dp, _ = dims
    seqs = tp * rows // dp
    width, state = w_x.shape[2], w_b.shape[2]
    both = width + 2 * padded(state)
    bf, f32, dma = jnp.bfloat16, jnp.float32, pltpu.SemaphoreType.DMA
    weights = [
        pltpu.VMEM((block, width), bf),
        pltpu.VMEM((block, width), bf),
        pltpu.VMEM((block, state), bf),
        pltpu.VMEM((block, state), bf),
        pltpu.VMEM((dt_width, block), bf),
    ]
    rest = [
        pltpu.VMEM((tp, rows, block), bf),
        pltpu.VMEM((dp, seqs, width + both), f32),
        pltpu.VMEM((dp, seqs, width), bf),
        pltpu.VMEM((dp, seqs, both), bf),
        pltpu.VMEM((dp - 1, seqs, width), bf),
        pltpu.VMEM((dp - 1, seqs, both), bf),
        pltpu.VMEM((dp, seqs, 2 * LANES), f32),
        pltpu.VMEM((dp - 1, seqs, 2 * LANES), f32),
        dma((tp,)),
        dma((tp,)),
        dma((3, dp)),
        dma((3, dp)),
        dma((5,)),
    ]
    return weights + rest


def back_scratch(dims, rows, block, width):
    tp, dp, _ = dims
    seqs = tp * rows // dp
    bf, f32, dma = jnp.bfloat16, jnp.float32, pltpu.SemaphoreType.DMA
    return [
        pltpu.VMEM((width, block), bf),
        pltpu.VMEM((dp, seqs, width), bf),
        pltpu.VMEM((tp, rows, block), f32),
        pltpu.VMEM((tp, rows, block), bf),
        pltpu.VMEM((tp - 1, rows, block), bf),
        dma((dp,)),
        dma((dp,)),
        dma((tp,)),
        dma((tp,)),
        dma((1,)),
    ]


FRONT = 18
BACK = 10


def split_front(refs):
    wz, wx, wb, wc, wdt, gathered, total, h0, h1, g0, g1, side, side_got = refs[:13]
    scratch = (wz, wx, wb, wc, wdt, gathered, total, (h0, h1), (g0, g1), side, side_got)
    return scratch + (refs[13:17],), refs[17]


def kernel(dims, layer, has_back, has_front, *refs):
    tp, dp, _ = dims
    refs = list(refs)
    take = lambda n: [refs.pop(0) for _ in range(n)]
    rows_ref = take(1)[0]
    if has_back:
        mixed_ref, wo_ref = take(2)
    if has_front:
        gain_ref, *weights = take(6)
    new_ref = take(1)[0] if has_back else rows_ref
    outs = take(2) if has_front else None
    back_refs = take(BACK) if has_back else None
    front_refs = take(FRONT) if has_front else None
    if has_back:
        load = pltpu.make_async_copy(wo_ref.at[layer], back_refs[0], back_refs[-1].at[0])
        load.start()
    if has_front:
        scratch, load_sems = split_front(front_refs)
        here = layer + 1 if has_back else layer
        loads = start_loads(here, list(zip(weights, scratch[:5])), load_sems)
    enter((("tp", tp), ("dp", dp)))
    if has_back:
        pieces = tuple(back_refs[:5]) + (back_refs[5:9],)
        back(dims, mixed_ref, rows_ref, load, pieces, new_ref)
    if has_front:
        front(dims, here, new_ref, gain_ref, loads, scratch, outs)


def exchange(dims, number, layer, rows, mixed, w_out, norm_gain, weights):
    has_back, has_front = mixed is not None, weights is not None
    tp, dp, _ = dims
    count, block = rows.shape
    seqs = tp * count // dp
    operands, specs, shapes, scratch = [rows], [VMEM], [], []
    if has_back:
        operands += [mixed, w_out]
        specs += [VMEM, HBM]
        shapes.append(jax.ShapeDtypeStruct(rows.shape, jnp.bfloat16))
        scratch += back_scratch(dims, count, block, mixed.shape[1])
    if has_front:
        operands += [norm_gain, *weights]
        specs += [VMEM] + [HBM] * 5
        w_x, w_b, w_dt = weights[1], weights[2], weights[4]
        across = 2 * w_x.shape[2] + 2 * padded(w_b.shape[2])
        shapes.append(jax.ShapeDtypeStruct((seqs, across), jnp.bfloat16))
        shapes.append(jax.ShapeDtypeStruct((seqs, LANES), jnp.float32))
        scratch += front_scratch(dims, count, block, w_x, w_b, w_dt.shape[1])
    return pl.pallas_call(
        functools.partial(kernel, dims, layer, has_back, has_front),
        out_shape=shapes,
        in_specs=specs,
        out_specs=[VMEM] * len(shapes),
        scratch_shapes=scratch,
        compiler_params=pltpu.CompilerParams(
            collective_id=number, has_side_effects=True, vmem_limit_bytes=56 * 2**20
        ),
    )(*operands)


def convolve(history_ref, latest, taps_ref, layer, kept_ref):
    weight = taps_ref[layer].astype(jnp.float32)
    old = history_ref.shape[1]
    summed = latest.astype(jnp.float32) * weight[old : old + 1]
    for k in range(old):
        summed = summed + history_ref[0, k].astype(jnp.float32) * weight[k : k + 1]
    for k in range(1, old):
        kept_ref[0, k - 1] = history_ref[0, k]
    kept_ref[0, old - 1] = latest
    return summed * jax.nn.sigmoid(summed)


def mix_kernel(layer, heads_step, aliased, *refs):
    act, steps, tap_x, tap_b, tap_c, bias, rate, skip, gain, prev, old_x, old_b, old_c = refs[:13]
    mixed, state, kept_x, kept_b, kept_c = refs[13 + aliased : 18 + aliased]
    skipped, factors, b_rows, c_rows, read = refs[18 + aliased :]
    seqs, width = mixed.shape
    heads = bias.shape[1]
    groups = b_rows.shape[0]
    per_group = heads // groups
    state_width = kept_b.shape[3]
    at = pl.program_id(0)

    @pl.when(at == 0)
    def _():
        raw = steps[:, 0:heads] + bias[layer : layer + 1, :]
        size = jnp.maximum(raw, 0.0) + jnp.log1p(jnp.exp(-jnp.abs(raw)))
        decay = jnp.exp(-size * jnp.exp(rate[layer : layer + 1, :]))
        skips = jnp.broadcast_to(skip[layer : layer + 1, :], (8, heads))
        stacked = jnp.concatenate([size, decay, skips], axis=0)
        row = lax.broadcasted_iota(jnp.int32, (heads, width), 0)
        lane = lax.broadcasted_iota(jnp.int32, (heads, width), 1)
        first = row * HEAD_DIM
        spread = jnp.where((lane >= first) & (lane < first + HEAD_DIM), 1.0, 0.0)
        wide = jnp.dot(
            stacked, spread, precision=lax.Precision.HIGHEST, preferred_element_type=jnp.float32
        )
        conv = convolve(old_x, act[:, width : 2 * width], tap_x, layer, kept_x)
        skipped[...] = wide[2 * seqs : 2 * seqs + 1] * conv
        both = jnp.concatenate([wide[0:seqs] * conv, wide[seqs : 2 * seqs]], axis=0)
        factors[...] = both.T
        begin = 2 * width
        for target, old, tap, kept in ((b_rows, old_b, tap_b, kept_b), (c_rows, old_c, tap_c, kept_c)):
            conv = convolve(old, act[:, begin : begin + state_width], tap, layer, kept)
            for g in range(groups):
                target[g] = conv[:, g * STATE : (g + 1) * STATE]
            begin += padded(state_width)

    group = at * heads_step // per_group
    b_here, c_half = b_rows[group], c_rows[group].astype(jnp.bfloat16)
    spot = lax.broadcasted_iota(jnp.int32, (HEAD_DIM, seqs), 1)
    for j in range(heads_step):
        first = pl.multiple_of((at * heads_step + j) * HEAD_DIM, HEAD_DIM)
        columns = factors[pl.ds(first, HEAD_DIM), :]
        taken = jnp.zeros((HEAD_DIM, seqs), jnp.float32)
        for s in range(seqs):
            fade = columns[0:1, seqs + s : seqs + s + 1]
            new = fade * prev[0, s, j] + columns[:, s : s + 1] * b_here[s : s + 1, :]
            state[0, s, j] = new
            summed = lax.dot_general(
                new.astype(jnp.bfloat16),
                c_half,
                (((1,), (1,)), ((), ())),
                preferred_element_type=jnp.float32,
            )
            taken = jnp.where(spot == s, summed, taken)
        read[pl.ds(first, HEAD_DIM), :] = taken

    @pl.when(at == pl.num_programs(0) - 1)
    def _():
        gate = act[:, 0:width].astype(jnp.float32)
        gated = (read[...].T + skipped[...]) * (gate * jax.nn.sigmoid(gate))
        span = per_group * HEAD_DIM
        for g in range(groups):
            part = gated[:, g * span : (g + 1) * span]
            scale = lax.rsqrt(jnp.mean(part * part, axis=1, keepdims=True) + EPSILON)
            gains = gain[layer : layer + 1, g * span : (g + 1) * span].astype(jnp.float32)
            mixed[:, g * span : (g + 1) * span] = (part * scale * gains).astype(jnp.bfloat16)


def mix(layer, act, steps, params, state, olds, carried):
    seqs, heads = state.shape[1:3]
    width, state_width = olds[0].shape[3], olds[1].shape[3]
    groups = state_width // STATE
    per_group = heads // groups
    heads_step = 2 if per_group % 2 == 0 else 1
    seqs_dim = lambda ref: (1,) + ref.shape[1:]
    whole = lambda ref: pl.BlockSpec(ref.shape, lambda i, n=ref.ndim: (0,) * n)
    at_layer = lambda ref: pl.BlockSpec(seqs_dim(ref), lambda i, n=ref.ndim: (layer,) + (0,) * (n - 1))
    tile = pl.BlockSpec(
        (1, seqs, heads_step, HEAD_DIM, STATE), lambda i: (layer, 0, i, 0, 0)
    )
    operands = [act, steps, *params, state, *olds]
    specs = [whole(x) for x in (act, steps, *params)] + [tile] + [at_layer(x) for x in olds]
    aliases = {}
    if carried is not None:
        aliases = {len(operands) + i: 1 + i for i in range(4)}
        operands += carried
        specs += [pl.BlockSpec(memory_space=pl.ANY)] * 4
    kinds = [jax.ShapeDtypeStruct(x.shape, x.dtype) for x in (state, *olds)]
    mixed = jax.ShapeDtypeStruct((seqs, width), jnp.bfloat16)
    f32 = jnp.float32
    return pl.pallas_call(
        functools.partial(mix_kernel, layer, heads_step, len(aliases)),
        grid=(heads // heads_step,),
        out_shape=[mixed] + kinds,
        in_specs=specs,
        out_specs=[whole(mixed), tile] + [at_layer(x) for x in olds],
        scratch_shapes=[
            pltpu.VMEM((seqs, width), f32),
            pltpu.VMEM((width, 2 * seqs), f32),
            pltpu.VMEM((groups, seqs, STATE), f32),
            pltpu.VMEM((groups, seqs, STATE), f32),
            pltpu.VMEM((width, seqs), f32),
        ],
        input_output_aliases=aliases,
        compiler_params=pltpu.CompilerParams(
            dimension_semantics=("arbitrary",), vmem_limit_bytes=56 * 2**20
        ),
    )(*operands)


def body(
    tokens,
    norm_gain,
    w_z,
    w_x,
    w_b,
    w_c,
    w_dt,
    conv_x,
    conv_b,
    conv_c,
    dt_bias,
    a_log,
    d_skip,
    out_gain,
    w_out,
    ssm_state,
    state_x,
    state_b,
    state_c,
):
    tp, dp = lax.axis_size("tp"), lax.axis_size("dp")
    dims = (tp, dp, tokens.shape[1] * dp)
    weights = (w_z, w_x, w_b, w_c, jnp.swapaxes(w_dt, 1, 2))
    layers = w_z.shape[0]
    params = (conv_x, conv_b, conv_c, dt_bias, a_log, d_skip, out_gain)
    olds = [jnp.swapaxes(x, 1, 2) for x in (state_x, state_b, state_c)]
    residual = tokens
    act, steps = exchange(dims, 0, 0, residual, None, None, norm_gain, weights)
    carried = None
    for layer in range(layers):
        mixed, *carried = mix(layer, act, steps, params, ssm_state, olds, carried)
        if layer + 1 < layers:
            residual, act, steps = exchange(
                dims, layer + 1, layer, residual, mixed, w_out, norm_gain, weights
            )
        else:
            (residual,) = exchange(dims, layer + 1, layer, residual, mixed, w_out, None, None)
    return (residual, carried[0], *(jnp.swapaxes(x, 1, 2) for x in carried[1:]))


def solution(mesh):
    placed = (
        P(("grp", "tp"), "dp"),
        P(None, "dp"),
        P(None, "dp", "tp"),
        P(None, "dp", "tp"),
        P(None, "dp", "tp"),
        P(None, "dp", "tp"),
        P(None, "dp", None),
        P(None, None, "tp"),
        P(None, None, "tp"),
        P(None, None, "tp"),
        P(None, "tp"),
        P(None, "tp"),
        P(None, "tp"),
        P(None, "tp"),
        P(None, "tp", "dp"),
        P(None, ("grp", "dp"), "tp", None, None),
        P(None, ("grp", "dp"), None, "tp"),
        P(None, ("grp", "dp"), None, "tp"),
        P(None, ("grp", "dp"), None, "tp"),
    )
    return jax.shard_map(
        body,
        mesh=mesh,
        in_specs=placed,
        out_specs=(
            P(("grp", "tp"), "dp"),
            P(None, ("grp", "dp"), "tp", None, None),
            P(None, ("grp", "dp"), None, "tp"),
            P(None, ("grp", "dp"), None, "tp"),
            P(None, ("grp", "dp"), None, "tp"),
        ),
        check_vma=False,
    )
```
